32 devices in a mesh: grp: 2 (over y), ep: 8 (over z, x), tp: 2 (over core).
Axes of the slice: x: 2, y: 2, z: 4, core: 2. Of those that a mesh axis runs over, the one named last changes fastest.
Arguments:
- tokens: bfloat16 [512, 2048], P(('grp', 'ep'), 'tp'), parts along dimension 0, may hold values from -6 to 6
- gain: float32 [2048], replicated, may hold values from 0.1 to 1.9
- routes: int32 [512, 4], P(('grp', 'ep')), parts along dimension 0, may hold values from 0 to 7, all different within a row; in each aligned block of 32 rows (0 to 31, 32 to 63, ...) at most 32 rows name the same one
- weights: float32 [512, 4], P(('grp', 'ep')), parts along dimension 0, may hold values from 0.05 to 1
- w_gate: bfloat16 [8, 2048, 6144], P('ep', None, 'tp'), may hold values from -0.125 to 0.125
- w_up: bfloat16 [8, 2048, 6144], P('ep', None, 'tp'), may hold values from -0.125 to 0.125
- w_down: bfloat16 [8, 6144, 2048], P('ep', 'tp'), may hold values from -0.078125 to 0.078125
Outputs:
- mixed: bfloat16 [512, 2048], P(('grp', 'ep'), 'tp'), parts along dimension 0
The draws below stay inside these ranges and needn't reach their ends.
There are 2 independent parts, one for each index of `grp`. The reference program is written for one: setup_inputs(seed, part) draws one part's arguments, and reference() takes and returns one part's arrays. A program takes and returns all parts, laid end to end along the dimension named above; an argument that names none is the same for every part. Nothing has to cross between parts.
Inputs may be any that keep to these rules, and one draw needn't show every extreme that they name: `routes`: each row names 4 different experts. Among the rows of one device no expert is named by more than 32 rows, a bound that some block reaches.
All inputs are finite; a program needn't handle non-finite values.
Results may differ from the reference program's by a relative error of at most 0.019.
Values may be sent and summed in bfloat16 or wider, within the bound.
No kernel may reach another device: no remote copies, remote signals or barrier semaphores. Data moves between devices by JAX's collectives and lax.ppermute only.
A program may use at most 128 MiB of HBM per device.

```python
import math
import jax
import jax.numpy as jnp
import numpy as np
from jax import lax

D = 2048
FF = 6144
TOP = 4
TOK_DEV = 32
EXPERTS = 8
CAP = 32
TOKENS = 256
N_EP = 8
N_TP = 2


def levels(own_key, shape, pieces, smallest, high):
    level = 1.0
    for axis_at, blocks in pieces:
        steps = jax.random.uniform(jax.random.fold_in(jax.random.fold_in(own_key, 6), axis_at), (blocks,), jnp.float32, smallest / len(pieces), high / len(pieces))
        level = level * jnp.repeat(jnp.exp(steps), shape[axis_at] // blocks).reshape((-1,) + (1,) * (len(shape) - 1 - axis_at))
    return level


def routed_block(rng, own, number, rows, number_of, top, most, skew):
    sequence = jax.random.permutation(rng, number_of)
    heavy_load, ordinary = portions_of(number_of, rows * top, most, skew, True), portions_of(number_of, rows * top, most, skew, False)
    places = jnp.arange(number_of)

    def named(tallies, offset_by):
        used = int((tallies > 0).sum())
        fixed = max(1, used // 4)
        moved = fixed + (places - fixed + offset_by * (used - fixed)) % max(1, number_of - fixed)
        return jnp.zeros((number_of,), jnp.int32).at[sequence[jnp.where(places < fixed, places, moved)]].set(jnp.asarray(tallies, jnp.int32))

    tallies = jnp.where(number % 4 == 0, named(heavy_load, number // 4), named(ordinary, number - number // 4 - 1))
    mixed = jax.random.permutation(jax.random.fold_in(own, 3), number_of)
    giver, receiver = mixed[0:number_of // 2 * 2:2], mixed[1:number_of // 2 * 2:2]
    slack = jnp.minimum(tallies[giver] - 1, most - tallies[receiver]) // 2
    slack = jnp.where((giver == sequence[0]) | (receiver == sequence[0]) | (tallies[receiver] == 0), 0, jnp.maximum(slack, 0))
    moved = jax.random.randint(jax.random.fold_in(own, 4), (number_of // 2,), 0, 1 << 20) % (slack + 1)
    tallies = tallies.at[giver].add(-moved).at[receiver].add(moved)
    items = jnp.searchsorted(jnp.cumsum(tallies), jnp.arange(rows * top), side="right").astype(jnp.int32)
    listing = items.reshape(top, rows).T
    listing = listing[jax.random.permutation(jax.random.fold_in(own, 1), rows)]
    offset_by = jax.random.randint(jax.random.fold_in(own, 2), (rows, 1), 0, top)
    return jnp.take_along_axis(listing, (jnp.arange(top)[None, :] + offset_by) % top, axis=1)


def portions_of(count, total, most, lean, full):
    weights = [(1 << 20) // math.isqrt(grade ** lean) + 1 for grade in range(1, count + 1)]
    largest = most if full else min(most, max(-(-total // count), total * weights[0] // sum(weights)))
    least = 1 if total - largest >= count - 1 else 0
    given, surplus = [largest] + [least] * (count - 1), total - largest - least * (count - 1)
    while surplus > 0:
        free = [i for i in range(1, count) if given[i] < largest] or [i for i in range(1, count) if given[i] < most]
        whole, budget = sum([weights[i] for i in free]), surplus
        for i in free:
            extra = min(most - given[i], max(1, budget * weights[i] // whole), surplus)
            given[i] = given[i] + extra
            surplus = surplus - extra
    return np.array(given)


def noise(rng, shape, scale, limit, split=(), held_as=jnp.bfloat16):
    result = scale * jax.random.normal(rng, shape, jnp.float32)
    if split:
        result = result * levels(rng, shape, split, -0.22, 0.18)
    return jnp.clip(result, -limit, limit).astype(held_as)


def setup_inputs(seed: int = 0, part: int = 0) -> dict:
    seeds = jax.random.split(jax.random.key(seed), 8)
    own_keys = jax.random.split(jax.random.fold_in(seeds[7], part), 8)
    tokens = noise(own_keys[0], (TOKENS, D), 1.0, 6.0, ((0, 8), (1, 2)))
    gain = jnp.clip(1.0 + 0.18 * jax.random.normal(seeds[1], (D,), jnp.float32), 0.1, 1.9)
    routes_keys = jax.random.split(jax.random.fold_in(own_keys[2], 1), TOKENS // TOK_DEV)
    routes_turns = jax.random.permutation(jax.random.fold_in(own_keys[2], 3), TOKENS // TOK_DEV)
    routes = jax.vmap(lambda own, number: routed_block(jax.random.fold_in(own_keys[2], 2), own, number, TOK_DEV, EXPERTS, TOP, CAP, 2))(routes_keys, routes_turns).reshape((TOKENS, TOP))
    weights = jnp.clip(jnp.exp(math.log(1.0) - 2.9957323 * jax.random.uniform(own_keys[3], (TOKENS, TOP), jnp.float32) ** levels(own_keys[3], (TOKENS, TOP), ((0, 8),), -0.2, 0.2)), 0.05, 1.0)
    w_gate = noise(seeds[4], (EXPERTS, D, FF), D ** -0.5, 0.125, ((0, 8), (2, 2)))
    w_up = noise(seeds[5], (EXPERTS, D, FF), D ** -0.5, 0.125, ((0, 8), (2, 2)))
    w_down = noise(seeds[6], (EXPERTS, FF, D), FF ** -0.5, 0.078125, ((0, 8), (1, 2)))
    return {"tokens": tokens, "gain": gain, "routes": routes, "weights": weights, "w_gate": w_gate, "w_up": w_up, "w_down": w_down}


epsilon = 1e-05

def normalize(values, gain):
    values = values.astype(jnp.float32)
    average = lax.optimization_barrier(jnp.mean(values, axis=1, keepdims=True))
    spread = lax.optimization_barrier(jnp.mean(jnp.square(values - average), axis=1, keepdims=True))
    return ((values - average) * lax.rsqrt(spread + epsilon) * gain).astype(jnp.bfloat16)

def reference(tokens, gain, routes, weights, w_gate, w_up, w_down):
    normed = normalize(tokens, gain)
    pair_count = TOKENS * TOP
    pair_expert = routes.reshape(-1).astype(jnp.int32)
    member = (pair_expert[:, None] == jnp.arange(EXPERTS, dtype=jnp.int32)[None, :]).astype(jnp.int32)
    earlier = jnp.cumsum(member, axis=0) - member
    room = N_EP * CAP
    position = (pair_expert * room + lax.optimization_barrier(jnp.sum(earlier * member, axis=1))).astype(jnp.int32)
    owner = jnp.full((EXPERTS * room,), TOKENS, jnp.int32)
    owner = owner.at[position].set(jnp.arange(pair_count, dtype=jnp.int32) // TOP)
    padded = jnp.concatenate([normed, jnp.zeros((1, D), jnp.bfloat16)], axis=0)
    block_width = FF // N_TP

    def expert(operands):
        index, gate_w, up_w, down_w = operands
        chosen = padded[index]
        gate_val = jnp.dot(chosen, gate_w, preferred_element_type=jnp.float32)
        up_val = jnp.dot(chosen, up_w, preferred_element_type=jnp.float32)
        hidden = (jax.nn.silu(gate_val) * up_val).astype(jnp.bfloat16)
        hidden_blocks = hidden.reshape(room, N_TP, block_width)
        down_blocks = down_w.reshape(N_TP, block_width, D)

        def one_block(carry, block):
            part = jnp.dot(block[0], block[1], preferred_element_type=jnp.float32).astype(jnp.bfloat16)
            return (carry + part.astype(jnp.float32), None)
        total, unused = lax.scan(one_block, jnp.zeros((room, D), jnp.float32), (jnp.swapaxes(hidden_blocks, 0, 1), down_blocks))
        return total.astype(jnp.bfloat16)
    results = lax.map(expert, (owner.reshape(EXPERTS, room), w_gate, w_up, w_down))
    results = results.reshape(EXPERTS * room, D)
    picked = results[position].reshape(TOKENS, TOP, D).astype(jnp.float32)
    return lax.optimization_barrier(jnp.sum(picked * weights[:, :, None], axis=1)).astype(jnp.bfloat16)
```

```python
import jax
import jax.numpy as jnp
from jax import lax
from jax.experimental import pallas as pl
from jax.experimental.pallas import tpu as pltpu
from jax.sharding import PartitionSpec as P

EPS = 1e-05
LANES = 128
MIB = 1 << 20


def vmem():
    return pl.BlockSpec(memory_space=pltpu.VMEM)


def hbm():
    return pl.BlockSpec(memory_space=pltpu.HBM)


def in_hbm(value):
    return pltpu.with_memory_space_constraint(value, pltpu.HBM)


def in_vmem(value):
    return pltpu.with_memory_space_constraint(value, pltpu.VMEM)


def block_of(size, most):
    return max(b for b in range(LANES, most + 1, LANES) if size % b == 0)


def swap(value, axis, bit):
    return lax.ppermute(value, axis, [(i, i ^ bit) for i in range(lax.axis_size(axis))])


def prepare_body(tokens_hbm, routes_hbm, weights_hbm, out, tokens, routes, weights, sem):
    copies = [
        pltpu.make_async_copy(a, b, sem.at[i])
        for i, (a, b) in enumerate(
            ((routes_hbm, routes), (weights_hbm, weights), (tokens_hbm, tokens))
        )
    ]
    for copy in copies:
        copy.start()
    copies[0].wait()
    copies[1].wait()
    rows, width = tokens.shape
    lane = lax.broadcasted_iota(jnp.int32, (LANES, rows), 0)
    share = jnp.zeros((LANES, rows), jnp.float32)
    for k in range(routes.shape[0]):
        share = share + jnp.where(routes[k : k + 1, :] == lane, weights[k : k + 1, :], 0.0)
    out[:, width:] = share.T.astype(jnp.bfloat16)
    copies[2].wait()
    out[:, :width] = tokens[...]


def prepare(tokens, routes, weights):
    rows, width = tokens.shape
    arrays = (tokens, routes.T, weights.T)
    return pl.pallas_call(
        prepare_body,
        out_shape=jax.ShapeDtypeStruct((rows, width + LANES), jnp.bfloat16),
        in_specs=[hbm()] * 3,
        out_specs=vmem(),
        scratch_shapes=[pltpu.VMEM(a.shape, a.dtype) for a in arrays]
        + [pltpu.SemaphoreType.DMA((3,))],
        compiler_params=pltpu.CompilerParams(vmem_limit_bytes=2 * MIB),
        name="prepare",
    )(*(in_hbm(a) for a in arrays))


def fetch_body(source, target, sem):
    copy = pltpu.make_async_copy(source, target, sem)
    copy.start()
    copy.wait()


def fetch(weight, after):
    del after
    return pl.pallas_call(
        fetch_body,
        out_shape=pltpu.VMEM(weight.shape, weight.dtype),
        in_specs=[hbm()],
        out_specs=vmem(),
        scratch_shapes=[pltpu.SemaphoreType.DMA],
        cost_estimate=pl.CostEstimate(
            flops=4 * 10**9, transcendentals=0, bytes_accessed=2 * weight.size
        ),
        compiler_params=pltpu.CompilerParams(vmem_limit_bytes=MIB),
        name="fetch",
    )(in_hbm(weight))


def expert_body(own, other, gain_hbm, w_gate, w_up, down, *rest, pieces, width, fetches):
    if fetches:
        keep, send, w_down, normed, hidden, gain, sem = rest
        copy = pltpu.make_async_copy(down, w_down, sem.at[1])
        copy.start()
    else:
        keep, send, normed, hidden, gain, sem = rest
        w_down = down
    gain_copy = pltpu.make_async_copy(gain_hbm, gain, sem.at[0])
    gain_copy.start()
    core, index = lax.axis_index("tp"), lax.axis_index("ep")
    at = pl.multiple_of(core * width, LANES)
    far = pl.multiple_of((pieces - 1 - core) * width, LANES)
    features = pieces * width
    mine = own[:, :width].astype(jnp.float32)
    theirs = other[:, :width].astype(jnp.float32)
    average = (
        jnp.sum(mine, axis=1, keepdims=True) + jnp.sum(theirs, axis=1, keepdims=True)
    ) / features
    mine = mine - average
    theirs = theirs - average
    spread = (
        jnp.sum(mine * mine, axis=1, keepdims=True)
        + jnp.sum(theirs * theirs, axis=1, keepdims=True)
    ) / features
    scale = lax.rsqrt(spread + EPS)
    gain_copy.wait()
    normed[:, pl.ds(at, width)] = (mine * scale * gain[:, pl.ds(at, width)]).astype(jnp.bfloat16)
    normed[:, pl.ds(far, width)] = (theirs * scale * gain[:, pl.ds(far, width)]).astype(
        jnp.bfloat16
    )
    share = own[:, width:].astype(jnp.float32)
    lane = lax.broadcasted_iota(jnp.int32, share.shape, 1)
    share = jnp.sum(jnp.where(lane == index, share, 0.0), axis=1, keepdims=True)
    chosen = normed[...]
    units = w_gate.shape[1]
    step = block_of(units, 256)
    for n in range(0, units, step):
        gate_val = jnp.dot(chosen, w_gate[:, n : n + step], preferred_element_type=jnp.float32)
        up_val = jnp.dot(chosen, w_up[:, n : n + step], preferred_element_type=jnp.float32)
        hidden[:, n : n + step] = (gate_val / (1.0 + jnp.exp(-gate_val)) * up_val).astype(
            jnp.bfloat16
        )
    if fetches:
        copy.wait()
    middle = hidden[...]
    step = block_of(width, 256)
    for target, base in ((send, far), (keep, at)):
        for n in range(0, width, step):
            part = jnp.dot(
                middle,
                w_down[:, pl.ds(pl.multiple_of(base + n, LANES), step)],
                preferred_element_type=jnp.float32,
            )
            target[:, n : n + step] = (part * share).astype(target.dtype)


def expert(own, other, gain, w_gate, w_up, w_down, fetches):
    width = own.shape[1] - LANES
    rows = own.shape[0]
    features, units = w_gate.shape
    body = lambda *refs: expert_body(
        *refs, pieces=features // width, width=width, fetches=fetches
    )
    rows_out = jax.ShapeDtypeStruct((rows, width), jnp.bfloat16)
    out_shape = [rows_out, rows_out]
    if fetches:
        out_shape.append(pltpu.VMEM(w_down.shape, w_down.dtype))
    return pl.pallas_call(
        body,
        out_shape=out_shape,
        in_specs=[vmem()] * 2 + [hbm()] + [vmem()] * 2 + [hbm() if fetches else vmem()],
        out_specs=[vmem()] * len(out_shape),
        scratch_shapes=[
            pltpu.VMEM((rows, features), jnp.bfloat16),
            pltpu.VMEM((rows, units), jnp.bfloat16),
            pltpu.VMEM((1, features), jnp.float32),
            pltpu.SemaphoreType.DMA((2,)),
        ],
        cost_estimate=pl.CostEstimate(
            flops=6 * rows * features * units,
            transcendentals=rows * units,
            bytes_accessed=6 * features * units,
        ),
        compiler_params=pltpu.CompilerParams(vmem_limit_bytes=12 * MIB),
        name="expert",
    )(
        own,
        other,
        in_hbm(gain[None, :]),
        in_vmem(w_gate),
        in_vmem(w_up),
        in_hbm(w_down) if fetches else in_vmem(w_down),
    )


def add(a, b):
    return (a.astype(jnp.float32) + b.astype(jnp.float32)).astype(jnp.bfloat16)


def on_device_pair(tokens, gain, routes, weights, w_gate, w_up, w_down):
    groups = lax.axis_size("ep")
    gathered = prepare(tokens, routes, weights)
    bits = []
    bit = groups // 2
    while bit > 1:
        gathered = jnp.concatenate([gathered, swap(gathered, "ep", bit)], axis=0)
        bits.append(bit)
        bit //= 2
    gate_w = fetch(w_gate[0], None)
    up_w = fetch(w_up[0], None)
    near = gathered
    near_other = swap(near, "tp", 1)
    beside = swap(near, "ep", 1)
    near_keep, near_send, down_w = expert(near, near_other, gain, gate_w, up_w, w_down[0], True)
    beside_other = swap(beside, "tp", 1)
    beside_keep, beside_send = expert(beside, beside_other, gain, gate_w, up_w, down_w, False)
    beside_sum = add(beside_keep, swap(beside_send, "tp", 1))
    near_sum = add(near_keep, swap(near_send, "tp", 1))
    total = add(near_sum, swap(beside_sum, "ep", 1))
    for bit in reversed(bits):
        half = total.shape[0] // 2
        total = add(total[:half], swap(total[half:], "ep", bit))
    return total


def on_device_any(tokens, gain, routes, weights, w_gate, w_up, w_down):
    groups = lax.axis_size("ep")
    width = tokens.shape[1]
    rows = prepare(tokens, routes, weights)
    bits = [1 << i for i in reversed(range(groups.bit_length() - 1))]
    for bit in bits:
        rows = jnp.concatenate([rows, swap(rows, "ep", bit)], axis=0)
    lane = jnp.arange(LANES, dtype=jnp.int32)[None, :]
    share = jnp.where(lane == lax.axis_index("ep"), rows[:, width:].astype(jnp.float32), 0.0)
    share = jnp.sum(share, axis=1, keepdims=True)
    values = lax.all_gather(rows[:, :width], "tp", axis=1, tiled=True).astype(jnp.float32)
    values = values - jnp.mean(values, axis=1, keepdims=True)
    spread = jnp.mean(values * values, axis=1, keepdims=True)
    chosen = (values * lax.rsqrt(spread + EPS) * gain).astype(jnp.bfloat16)
    gate_val = jnp.dot(chosen, w_gate[0], preferred_element_type=jnp.float32)
    up_val = jnp.dot(chosen, w_up[0], preferred_element_type=jnp.float32)
    hidden = (jax.nn.silu(gate_val) * up_val).astype(jnp.bfloat16)
    part = jnp.dot(hidden, w_down[0], preferred_element_type=jnp.float32)
    total = lax.psum_scatter(
        (part * share).astype(jnp.bfloat16), "tp", scatter_dimension=1, tiled=True
    )
    for bit in reversed(bits):
        half = total.shape[0] // 2
        total = add(total[:half], swap(total[half:], "ep", bit))
    return total


def solution(mesh):
    in_specs = (
        P(("grp", "ep"), "tp"),
        P(),
        P(("grp", "ep"), None),
        P(("grp", "ep"), None),
        P("ep", None, "tp"),
        P("ep", None, "tp"),
        P("ep", "tp", None),
    )
    on_device = on_device_pair if mesh.shape["tp"] == 2 else on_device_any
    return jax.shard_map(
        on_device,
        mesh=mesh,
        in_specs=in_specs,
        out_specs=P(("grp", "ep"), "tp"),
        check_vma=False,
    )
```

```python
import jax
import jax.numpy as jnp
from jax import lax
from jax.experimental import pallas as pl
from jax.experimental.pallas import tpu as pltpu
from jax.sharding import PartitionSpec as P


EPS = 1e-05
LANES = 128
MIB = 1 << 20


def vmem():
    return pl.BlockSpec(memory_space=pltpu.VMEM)


def hbm():
    return pl.BlockSpec(memory_space=pltpu.HBM)


def in_hbm(value):
    return pltpu.with_memory_space_constraint(value, pltpu.HBM)


def in_vmem(value):
    return pltpu.with_memory_space_constraint(value, pltpu.VMEM)


def cost(flops):
    return pl.CostEstimate(flops=flops, transcendentals=0, bytes_accessed=flops // 256)


def block_of(size, most):
    return max(b for b in range(LANES, most + 1, LANES) if size % b == 0)


def swap(value, axis, bit):
    return lax.ppermute(value, axis, [(i, i ^ bit) for i in range(lax.axis_size(axis))])


def prepare_body(tokens_hbm, routes_hbm, weights_hbm, out, tokens, routes, weights, sem):
    copies = [
        pltpu.make_async_copy(a, b, sem.at[i])
        for i, (a, b) in enumerate(
            ((routes_hbm, routes), (weights_hbm, weights), (tokens_hbm, tokens))
        )
    ]
    for copy in copies:
        copy.start()
    copies[0].wait()
    copies[1].wait()
    rows, width = tokens.shape
    lane = lax.broadcasted_iota(jnp.int32, (LANES, rows), 0)
    share = jnp.zeros((LANES, rows), jnp.float32)
    for k in range(routes.shape[0]):
        share = share + jnp.where(routes[k : k + 1, :] == lane, weights[k : k + 1, :], 0.0)
    out[:, width:] = share.T.astype(jnp.bfloat16)
    copies[2].wait()
    out[:, :width] = tokens[...]


def prepare(tokens, routes, weights):
    rows, width = tokens.shape
    arrays = (tokens, routes.T, weights.T)
    return pl.pallas_call(
        prepare_body,
        out_shape=jax.ShapeDtypeStruct((rows, width + LANES), jnp.bfloat16),
        in_specs=[hbm()] * 3,
        out_specs=vmem(),
        scratch_shapes=[pltpu.VMEM(a.shape, a.dtype) for a in arrays]
        + [pltpu.SemaphoreType.DMA((3,))],
        cost_estimate=cost(12 * 10**9),
        compiler_params=pltpu.CompilerParams(vmem_limit_bytes=2 * MIB),
        name="prepare",
    )(*(in_hbm(a) for a in arrays))


def half_at(far, width):
    core = lax.axis_index("tp")
    return pl.multiple_of((1 - core if far else core) * width, LANES)


def up_body(own, other, gain_hbm, w_gate, w_up, hidden, normed, gain, sem, *, width):
    gain_copy = pltpu.make_async_copy(gain_hbm, gain, sem)
    gain_copy.start()
    at = half_at(False, width)
    far = half_at(True, width)
    features = 2 * width
    mine = own[:, :width].astype(jnp.float32)
    theirs = other[:, :width].astype(jnp.float32)
    average = (
        jnp.sum(mine, axis=1, keepdims=True) + jnp.sum(theirs, axis=1, keepdims=True)
    ) / features
    mine = mine - average
    theirs = theirs - average
    spread = (
        jnp.sum(mine * mine, axis=1, keepdims=True)
        + jnp.sum(theirs * theirs, axis=1, keepdims=True)
    ) / features
    scale = lax.rsqrt(spread + EPS)
    gain_copy.wait()
    normed[:, pl.ds(at, width)] = (mine * scale * gain[:, pl.ds(at, width)]).astype(jnp.bfloat16)
    normed[:, pl.ds(far, width)] = (theirs * scale * gain[:, pl.ds(far, width)]).astype(
        jnp.bfloat16
    )
    chosen = normed[...]
    units = w_gate.shape[1]
    step = block_of(units, 512)
    for n in range(0, units, step):
        gate_val = jnp.dot(chosen, w_gate[:, n : n + step], preferred_element_type=jnp.float32)
        up_val = jnp.dot(chosen, w_up[:, n : n + step], preferred_element_type=jnp.float32)
        hidden[:, n : n + step] = (gate_val / (1.0 + jnp.exp(-gate_val)) * up_val).astype(
            jnp.bfloat16
        )


def project_up(own, other, gain, w_gate, w_up):
    rows, width = own.shape[0], own.shape[1] - LANES
    features, units = w_gate.shape
    return pl.pallas_call(
        lambda *refs: up_body(*refs, width=width),
        out_shape=jax.ShapeDtypeStruct((rows, units), jnp.bfloat16),
        in_specs=[vmem()] * 2 + [hbm()] + [vmem()] * 2,
        out_specs=vmem(),
        scratch_shapes=[
            pltpu.VMEM((rows, features), jnp.bfloat16),
            pltpu.VMEM((1, features), jnp.float32),
            pltpu.SemaphoreType.DMA,
        ],
        cost_estimate=cost(4 * rows * features * units),
        compiler_params=pltpu.CompilerParams(vmem_limit_bytes=8 * MIB),
        name="up",
    )(own, other, in_hbm(gain[None, :]), in_vmem(w_gate), in_vmem(w_up))


def down_body(own, hidden, w_down, out, *, far):
    width = out.shape[1]
    share = own[:, width:].astype(jnp.float32)
    lane = lax.broadcasted_iota(jnp.int32, share.shape, 1)
    share = jnp.sum(
        jnp.where(lane == lax.axis_index("ep"), share, 0.0), axis=1, keepdims=True
    )
    middle = hidden[...]
    step = block_of(width, 512)
    base = half_at(far, width)
    for n in range(0, width, step):
        part = jnp.dot(
            middle,
            w_down[:, pl.ds(pl.multiple_of(base + n, LANES), step)],
            preferred_element_type=jnp.float32,
        )
        out[:, n : n + step] = (part * share).astype(out.dtype)


def project_down(own, hidden, w_down, far):
    rows, units = hidden.shape
    width = own.shape[1] - LANES
    return pl.pallas_call(
        lambda *refs: down_body(*refs, far=far),
        out_shape=jax.ShapeDtypeStruct((rows, width), jnp.bfloat16),
        in_specs=[vmem()] * 3,
        out_specs=vmem(),
        cost_estimate=cost(2 * rows * units * width),
        compiler_params=pltpu.CompilerParams(vmem_limit_bytes=6 * MIB),
        name="down",
    )(own, hidden, in_vmem(w_down))


def add(*parts):
    return sum(p.astype(jnp.float32) for p in parts).astype(jnp.bfloat16)


def on_device_pair(tokens, gain, routes, weights, w_gate, w_up, w_down):
    return step_pair(tokens, gain, routes, weights, w_gate[0], w_up[0], w_down[0])


def step_pair(tokens, gain, routes, weights, w_gate, w_up, w_down):
    groups = lax.axis_size("ep")
    rows = tokens.shape[0]
    mine = prepare(tokens, routes, weights)
    column = sorted(range(2, groups, 2), key=lambda k: f"{k:b}"[::-1])
    near = [mine] + [swap(mine, "ep", k) for k in column]
    near = jnp.concatenate(near, axis=0)
    near_other = swap(near, "tp", 1)
    beside = swap(near, "ep", 1)
    near_hidden = project_up(near, near_other, gain, w_gate, w_up)
    near_send = project_down(near, near_hidden, w_down, True)
    near_back = swap(near_send, "tp", 1)
    beside_other = swap(beside, "tp", 1)
    near_keep = project_down(near, near_hidden, w_down, False)
    near_sum = add(near_keep, near_back)
    beside_hidden = project_up(beside, beside_other, gain, w_gate, w_up)
    beside_send = project_down(beside, beside_hidden, w_down, True)
    beside_back = swap(beside_send, "tp", 1)
    beside_keep = project_down(beside, beside_hidden, w_down, False)
    beside_sum = add(beside_keep, beside_back)
    bit = 1
    while near_sum.shape[0] > rows:
        half = near_sum.shape[0] // 2
        bit *= 2
        near_sum = add(near_sum[:half], swap(near_sum[half:], "ep", bit))
    parts = [near_sum]
    for i, k in enumerate([0] + column):
        block = beside_sum[i * rows : (i + 1) * rows]
        parts.append(swap(block, "ep", k + 1))
    return add(*parts)


def on_device_any(tokens, gain, routes, weights, w_gate, w_up, w_down):
    groups = lax.axis_size("ep")
    width = tokens.shape[1]
    rows = prepare(tokens, routes, weights)
    bits = [1 << i for i in reversed(range(groups.bit_length() - 1))]
    for bit in bits:
        rows = jnp.concatenate([rows, swap(rows, "ep", bit)], axis=0)
    lane = jnp.arange(LANES, dtype=jnp.int32)[None, :]
    share = jnp.where(lane == lax.axis_index("ep"), rows[:, width:].astype(jnp.float32), 0.0)
    share = jnp.sum(share, axis=1, keepdims=True)
    values = lax.all_gather(rows[:, :width], "tp", axis=1, tiled=True).astype(jnp.float32)
    values = values - jnp.mean(values, axis=1, keepdims=True)
    spread = jnp.mean(values * values, axis=1, keepdims=True)
    chosen = (values * lax.rsqrt(spread + EPS) * gain).astype(jnp.bfloat16)
    gate_val = jnp.dot(chosen, w_gate[0], preferred_element_type=jnp.float32)
    up_val = jnp.dot(chosen, w_up[0], preferred_element_type=jnp.float32)
    hidden = (jax.nn.silu(gate_val) * up_val).astype(jnp.bfloat16)
    part = jnp.dot(hidden, w_down[0], preferred_element_type=jnp.float32)
    total = lax.psum_scatter(
        (part * share).astype(jnp.bfloat16), "tp", scatter_dimension=1, tiled=True
    )
    for bit in reversed(bits):
        half = total.shape[0] // 2
        total = add(total[:half], swap(total[half:], "ep", bit))
    return total


def solution(mesh):
    in_specs = (
        P(("grp", "ep"), "tp"),
        P(),
        P(("grp", "ep"), None),
        P(("grp", "ep"), None),
        P("ep", None, "tp"),
        P("ep", None, "tp"),
        P("ep", "tp", None),
    )
    pair = mesh.shape["tp"] == 2 and mesh.shape["ep"] == 8
    return jax.shard_map(
        on_device_pair if pair else on_device_any,
        mesh=mesh,
        in_specs=in_specs,
        out_specs=P(("grp", "ep"), "tp"),
        check_vma=False,
    )
```

```python
import jax
import jax.numpy as jnp
from jax import lax
from jax.experimental import pallas as pl
from jax.experimental.pallas import tpu as pltpu
from jax.sharding import PartitionSpec as P


EPS = 1e-05
LANES = 128
MIB = 1 << 20


def vmem():
    return pl.BlockSpec(memory_space=pltpu.VMEM)


def hbm():
    return pl.BlockSpec(memory_space=pltpu.HBM)


def in_hbm(value):
    return pltpu.with_memory_space_constraint(value, pltpu.HBM)


def in_vmem(value):
    return pltpu.with_memory_space_constraint(value, pltpu.VMEM)


def cost(flops):
    return pl.CostEstimate(flops=flops, transcendentals=0, bytes_accessed=flops // 256)


def block_of(size, most):
    return max(b for b in range(LANES, most + 1, LANES) if size % b == 0)


def swap(value, axis, bit):
    return lax.ppermute(value, axis, [(i, i ^ bit) for i in range(lax.axis_size(axis))])


def share_body(routes_hbm, weights_hbm, out, routes, weights, sem):
    copies = [
        pltpu.make_async_copy(routes_hbm, routes, sem.at[0]),
        pltpu.make_async_copy(weights_hbm, weights, sem.at[1]),
    ]
    for copy in copies:
        copy.start()
    for copy in copies:
        copy.wait()
    top, rows = routes.shape
    expert = lax.broadcasted_iota(jnp.int32, (LANES, rows), 0) ^ lax.axis_index("ep")
    share = jnp.zeros((LANES, rows), jnp.float32)
    for k in range(top):
        share = share + jnp.where(routes[k : k + 1, :] == expert, weights[k : k + 1, :], 0.0)
    out[...] = share.T


def shares(routes, weights):
    arrays = (routes.T, weights.T)
    return pl.pallas_call(
        share_body,
        out_shape=jax.ShapeDtypeStruct((routes.shape[0], LANES), jnp.float32),
        in_specs=[hbm()] * 2,
        out_specs=vmem(),
        scratch_shapes=[pltpu.VMEM(a.shape, a.dtype) for a in arrays]
        + [pltpu.SemaphoreType.DMA((2,))],
        compiler_params=pltpu.CompilerParams(vmem_limit_bytes=2 * MIB),
        name="shares",
    )(*(in_hbm(a) for a in arrays))


def open_body(out):
    out[...] = jnp.zeros(out.shape, out.dtype)


def opening():
    return pl.pallas_call(
        open_body,
        out_shape=jax.ShapeDtypeStruct((8, LANES), jnp.float32),
        out_specs=vmem(),
        cost_estimate=cost(12 * 10**9),
        compiler_params=pltpu.CompilerParams(vmem_limit_bytes=MIB),
        name="opening",
    )()


def half_at(far, width):
    core = lax.axis_index("tp")
    return pl.multiple_of((1 - core if far else core) * width, LANES)


def up_body(own, other, gain_hbm, w_gate, w_up, hidden, normed, gain, sem, *, width):
    gain_copy = pltpu.make_async_copy(gain_hbm, gain, sem)
    gain_copy.start()
    at = half_at(False, width)
    far = half_at(True, width)
    features = 2 * width
    mine = own[:, :width].astype(jnp.float32)
    theirs = other[:, :width].astype(jnp.float32)
    average = (
        jnp.sum(mine, axis=1, keepdims=True) + jnp.sum(theirs, axis=1, keepdims=True)
    ) / features
    mine = mine - average
    theirs = theirs - average
    spread = (
        jnp.sum(mine * mine, axis=1, keepdims=True)
        + jnp.sum(theirs * theirs, axis=1, keepdims=True)
    ) / features
    scale = lax.rsqrt(spread + EPS)
    gain_copy.wait()
    normed[:, pl.ds(at, width)] = (mine * scale * gain[:, pl.ds(at, width)]).astype(jnp.bfloat16)
    normed[:, pl.ds(far, width)] = (theirs * scale * gain[:, pl.ds(far, width)]).astype(
        jnp.bfloat16
    )
    chosen = normed[...]
    units = w_gate.shape[1]
    step = block_of(units, 512)
    for n in range(0, units, step):
        gate_val = jnp.dot(chosen, w_gate[:, n : n + step], preferred_element_type=jnp.float32)
        up_val = jnp.dot(chosen, w_up[:, n : n + step], preferred_element_type=jnp.float32)
        hidden[:, n : n + step] = (gate_val / (1.0 + jnp.exp(-gate_val)) * up_val).astype(
            jnp.bfloat16
        )


def project_up(own, other, gain, w_gate, w_up):
    rows, width = own.shape
    features, units = w_gate.shape
    return pl.pallas_call(
        lambda *refs: up_body(*refs, width=width),
        out_shape=jax.ShapeDtypeStruct((rows, units), jnp.bfloat16),
        in_specs=[vmem()] * 2 + [hbm()] + [vmem()] * 2,
        out_specs=vmem(),
        scratch_shapes=[
            pltpu.VMEM((rows, features), jnp.bfloat16),
            pltpu.VMEM((1, features), jnp.float32),
            pltpu.SemaphoreType.DMA,
        ],
        cost_estimate=cost(4 * rows * features * units),
        compiler_params=pltpu.CompilerParams(vmem_limit_bytes=8 * MIB),
        name="up",
    )(own, other, in_hbm(gain[None, :]), in_vmem(w_gate), in_vmem(w_up))


def down_body(hidden, w_down, out, *, far):
    width = out.shape[1]
    middle = hidden[...]
    step = block_of(width, 512)
    base = half_at(far, width)
    for n in range(0, width, step):
        part = jnp.dot(
            middle,
            w_down[:, pl.ds(pl.multiple_of(base + n, LANES), step)],
            preferred_element_type=jnp.float32,
        )
        out[:, n : n + step] = part.astype(out.dtype)


def project_down(hidden, w_down, far):
    rows, units = hidden.shape
    width = w_down.shape[1] // 2
    return pl.pallas_call(
        lambda *refs: down_body(*refs, far=far),
        out_shape=jax.ShapeDtypeStruct((rows, width), jnp.bfloat16),
        in_specs=[vmem()] * 2,
        out_specs=vmem(),
        cost_estimate=cost(2 * rows * units * width),
        compiler_params=pltpu.CompilerParams(vmem_limit_bytes=6 * MIB),
        name="down",
    )(hidden, in_vmem(w_down))


def combine_body(zero, share, order, *refs):
    blocks, out, total, sem = refs[:-3], refs[-3], refs[-2], refs[-1]
    rows, width = total.shape
    copies = []
    step = block_of(width, 512)
    for n in range(0, width, step):
        part = jnp.tile(zero[...], (rows // 8, step // LANES))
        for k, block in zip(order, blocks):
            weight = share[:, k : k + 1]
            part = part + block[:rows, n : n + step].astype(jnp.float32) * weight
        total[:, n : n + step] = part.astype(total.dtype)
        copies.append(
            pltpu.make_async_copy(
                total.at[:, n : n + step], out.at[:, n : n + step], sem.at[n // step]
            )
        )
        copies[-1].start()
    for copy in copies:
        copy.wait()


def combine(zero, share, blocks):
    rows = share.shape[0]
    width = blocks[0][1].shape[1]
    order = [k for k, _ in blocks]
    values = [value for _, value in blocks]
    body = lambda zero, share, *refs: combine_body(zero, share, order, *refs)
    return pl.pallas_call(
        body,
        out_shape=jax.ShapeDtypeStruct((rows, width), jnp.bfloat16),
        in_specs=[vmem()] * (2 + len(values)),
        out_specs=hbm(),
        scratch_shapes=[
            pltpu.VMEM((rows, width), jnp.bfloat16),
            pltpu.SemaphoreType.DMA((width // block_of(width, 512),)),
        ],
        compiler_params=pltpu.CompilerParams(vmem_limit_bytes=2 * MIB),
        name="combine",
    )(zero, share, *values)


def add(*parts):
    return sum(p.astype(jnp.float32) for p in parts).astype(jnp.bfloat16)


def on_device_pair(tokens, gain, routes, weights, w_gate, w_up, w_down):
    return step_pair(tokens, gain, routes, weights, w_gate[0], w_up[0], w_down[0])


def step_pair(tokens, gain, routes, weights, w_gate, w_up, w_down):
    groups = lax.axis_size("ep")
    rows = tokens.shape[0]
    zero = opening()
    share = shares(routes, weights)
    column = range(2, groups, 2)
    near = [tokens] + [swap(tokens, "ep", k) for k in column]
    near = jnp.concatenate(near, axis=0)
    near_other = swap(near, "tp", 1)
    beside = swap(near, "ep", 1)
    near_hidden = project_up(near, near_other, gain, w_gate, w_up)
    near_send = project_down(near_hidden, w_down, True)
    near_back = swap(near_send, "tp", 1)
    beside_other = swap(beside, "tp", 1)
    near_keep = project_down(near_hidden, w_down, False)
    near_sum = add(near_keep, near_back)
    beside_hidden = project_up(beside, beside_other, gain, w_gate, w_up)
    beside_send = project_down(beside_hidden, w_down, True)
    beside_back = swap(beside_send, "tp", 1)
    beside_keep = project_down(beside_hidden, w_down, False)
    beside_sum = add(beside_keep, beside_back)
    blocks = []
    for first, result in ((0, near_sum), (1, beside_sum)):
        for i in range(groups // 2):
            k = 2 * i + first
            block = result[i * rows : (i + 1) * rows]
            blocks.append((k, swap(block, "ep", k) if k else result))
    return combine(zero, share, blocks)


def on_device_any(tokens, gain, routes, weights, w_gate, w_up, w_down):
    groups = lax.axis_size("ep")
    width = tokens.shape[1]
    experts = jnp.arange(LANES, dtype=jnp.int32)
    share = jnp.where(routes[:, :, None] == experts, weights[:, :, None], 0.0).sum(axis=1)
    rows = jnp.concatenate([tokens, share.astype(jnp.bfloat16)], axis=1)
    bits = [1 << i for i in reversed(range(groups.bit_length() - 1))]
    for bit in bits:
        rows = jnp.concatenate([rows, swap(rows, "ep", bit)], axis=0)
    share = jnp.where(experts == lax.axis_index("ep"), rows[:, width:].astype(jnp.float32), 0.0)
    share = jnp.sum(share, axis=1, keepdims=True)
    values = lax.all_gather(rows[:, :width], "tp", axis=1, tiled=True).astype(jnp.float32)
    values = values - jnp.mean(values, axis=1, keepdims=True)
    spread = jnp.mean(values * values, axis=1, keepdims=True)
    chosen = (values * lax.rsqrt(spread + EPS) * gain).astype(jnp.bfloat16)
    gate_val = jnp.dot(chosen, w_gate[0], preferred_element_type=jnp.float32)
    up_val = jnp.dot(chosen, w_up[0], preferred_element_type=jnp.float32)
    hidden = (jax.nn.silu(gate_val) * up_val).astype(jnp.bfloat16)
    part = jnp.dot(hidden, w_down[0], preferred_element_type=jnp.float32)
    total = lax.psum_scatter(
        (part * share).astype(jnp.bfloat16), "tp", scatter_dimension=1, tiled=True
    )
    for bit in reversed(bits):
        half = total.shape[0] // 2
        total = add(total[:half], swap(total[half:], "ep", bit))
    return total


def solution(mesh):
    in_specs = (
        P(("grp", "ep"), "tp"),
        P(),
        P(("grp", "ep"), None),
        P(("grp", "ep"), None),
        P("ep", None, "tp"),
        P("ep", None, "tp"),
        P("ep", "tp", None),
    )
    pair = mesh.shape["tp"] == 2 and mesh.shape["ep"] == 8
    return jax.shard_map(
        on_device_pair if pair else on_device_any,
        mesh=mesh,
        in_specs=in_specs,
        out_specs=P(("grp", "ep"), "tp"),
        check_vma=False,
    )
```
